512 devices in a mesh: fs: 64 (over z, y), tp: 8 (over x, core).
Axes of the slice: x: 4, y: 8, z: 8, core: 2. Of those that a mesh axis runs over, the one named last changes fastest.
Arguments:
- saved_input: bfloat16 [65536, 2048], P('fs'), may hold values from -60 to 60
- out_cotangent: bfloat16 [65536, 4096], P('fs', 'tp'), may hold values from -6 to 6
- old_weight: float32 [2048, 4096], P('fs', 'tp'), may hold values from -0.125 to 0.125
- factor: bfloat16 [4096, 256], P('tp'), may hold values from -0.09375 to 0.09375
- moment_first: float32 [2048, 256], P('fs'), may hold values from -3 to 3
- moment_second: float32 [2048, 256], P('fs'), may hold values from 0.05 to 1
Outputs:
- new_weight: float32 [2048, 4096], P('fs', 'tp')
- update: float32 [2048, 4096], P('fs', 'tp')
- new_first: float32 [2048, 256], P('fs')
- new_second: float32 [2048, 256], P('fs')
- weight_copy: bfloat16 [2048, 4096], P(None, 'tp')
The draws below stay inside these ranges and needn't reach their ends.
All inputs are finite; a program needn't handle non-finite values.
Results may differ from the reference program's by a relative error of at most 0.0028.
Values may be sent and summed in bfloat16 or wider, within the bound.
No kernel may reach another device: no remote copies, remote signals or barrier semaphores. Data moves between devices by JAX's collectives and lax.ppermute only.
A program may use at most 64 MiB of HBM per device.

```python
import math
import jax
import jax.numpy as jnp
from jax import lax

D = 4096
HV = 2048
RANK = 256
TOKENS = 65536


def draw_saved_input(key, part):
    first = jax.random.fold_in(jax.random.fold_in(key, 11), 0)
    column = jnp.arange(HV, dtype=jnp.float32) / HV
    scale = jnp.exp(column * 2.302585)
    values = jnp.clip(jax.random.normal(first, (TOKENS, HV), jnp.float32), -6.0, 6.0) * scale
    return values.astype(jnp.bfloat16)


def level_of(stream_key, extent, shards, least, largest):
    gain, own = 1.0, jax.random.fold_in(stream_key, 6)
    for position, parts in shards:
        draws = jnp.exp(jax.random.uniform(jax.random.fold_in(own, position), (parts,), jnp.float32, least / len(shards), largest / len(shards)))
        gain = gain * jnp.repeat(draws, extent[position] // parts).reshape([-1 if axis == position else 1 for axis in range(len(extent))])
    return gain


def noise(own_key, shape, width, limit, cuts=(), kind=jnp.bfloat16):
    values = jax.random.normal(own_key, shape, jnp.float32) * width
    if len(cuts) > 0:
        values = level_of(own_key, shape, cuts, -0.22, 0.18) * values
    return jnp.clip(values, min=-limit, max=limit).astype(kind)


def setup_inputs(seed: int = 0) -> dict:
    seeds = jax.random.split(jax.random.key(seed), 7)
    saved_input = draw_saved_input(jax.random.fold_in(seeds[6], 71), 0)
    out_cotangent = noise(seeds[1], (TOKENS, D), 1.0, 6.0, ((0, 64), (1, 8)))
    old_weight = noise(seeds[2], (HV, D), HV ** -0.5, 0.125, ((0, 64), (1, 8)), jnp.float32)
    factor = noise(seeds[3], (D, RANK), D ** -0.5, 0.09375, ((0, 8),))
    moment_first = noise(seeds[4], (HV, RANK), 0.5, 3.0, ((0, 64),), jnp.float32)
    moment_second = jnp.clip(jnp.exp(math.log(1.0) - 2.9957323 * jax.random.uniform(seeds[5], (HV, RANK), jnp.float32) ** level_of(seeds[5], (HV, RANK), ((0, 64),), -0.2, 0.2)), 0.05, 1.0)
    return {"saved_input": saved_input, "out_cotangent": out_cotangent, "old_weight": old_weight, "factor": factor, "moment_first": moment_first, "moment_second": moment_second}


def reference(saved_input, out_cotangent, old_weight, factor, moment_first, moment_second):
    gradient = jnp.dot(saved_input.T, out_cotangent, preferred_element_type=jnp.float32)
    wide_factor = factor.astype(jnp.float32)
    projected = jnp.dot(gradient, wide_factor, precision=lax.Precision.HIGHEST)
    total = jnp.sqrt(jnp.sum(projected * projected))
    clip = jnp.minimum(1.0, math.sqrt(HV * RANK) / (total + 1e-06))
    clipped = clip * projected
    new_first = 0.9 * moment_first + 0.1 * clipped
    new_second = 0.95 * moment_second + 0.05 * clipped * clipped
    direction = new_first / (jnp.sqrt(new_second) + 1e-08)
    update = jnp.dot(direction, wide_factor.T, precision=lax.Precision.HIGHEST)
    new_weight = old_weight - 0.05 * update
    return (new_weight, update, new_first, new_second, new_weight.astype(jnp.bfloat16))
```

```python
import math

import jax
import jax.numpy as jnp
from jax import lax
from jax.sharding import Mesh
from jax.sharding import PartitionSpec as P

HV = 2048
RANK = 256
FS = ("fs_0", "fs_1")


def exchanged(blocks, axis):
    return lax.all_to_all(blocks, axis, 0, 0, tiled=True)


def copy_for_each(shard, axis):
    devices = lax.axis_size(axis)
    return exchanged(jnp.broadcast_to(shard[None], (devices, *shard.shape)), axis)


def shifted(shard, axis, by):
    size = lax.axis_size(axis)
    return lax.ppermute(shard, axis, [(k, (k + by) % size) for k in range(size)])


def ring_gathered(shard, axis):
    size = lax.axis_size(axis)
    here = lax.axis_index(axis)
    half = shard.shape[0] // 2
    whole = jnp.zeros((size, *shard.shape), shard.dtype)

    def put(whole, block, at, row=0):
        return lax.dynamic_update_slice(whole, block[None], (at % size, row, 0))

    whole = put(whole, shard, here)
    up = down = shard
    for step in range(1, size // 2):
        up, down = shifted(up, axis, 1), shifted(down, axis, -1)
        whole = put(whole, up, here - step + size)
        whole = put(whole, down, here + step)
    far = here + size // 2
    whole = put(whole, shifted(up[:half], axis, 1), far)
    return put(whole, shifted(down[half:], axis, -1), far, half)


def on_device(saved_input, out_cotangent, old_weight, factor, moment_first, moment_second):
    fs, tp = lax.axis_size(FS), lax.axis_size("tp")
    rows = HV // fs
    contract = (((0,), (0,)), ((), ()))
    low = jnp.dot(out_cotangent, factor, preferred_element_type=jnp.float32)
    part = lax.dot_general(
        saved_input, low.astype(jnp.bfloat16), contract, preferred_element_type=jnp.float32
    )
    part = part.astype(jnp.bfloat16).reshape(fs, tp, rows // tp, RANK).transpose(1, 0, 2, 3)
    tiles = exchanged(part.reshape(tp, fs * rows // tp, RANK), "tp")
    part = jnp.sum(tiles.astype(jnp.float32), axis=0).reshape(fs, rows // tp, RANK)
    own = jnp.sum(exchanged(part, FS), axis=0)
    projected = copy_for_each(own, "tp").reshape(rows, RANK)
    squares = jnp.full((1, 128), jnp.sum(projected * projected), jnp.float32)
    squares = jnp.sum(copy_for_each(squares, FS)[:, 0, 0])
    clip = jnp.minimum(1.0, math.sqrt(HV * RANK) / (jnp.sqrt(squares) + 1e-06))
    clipped = clip * projected
    new_first = 0.9 * moment_first + 0.1 * clipped
    new_second = 0.95 * moment_second + 0.05 * clipped * clipped
    direction = new_first / (jnp.sqrt(new_second) + 1e-08)
    update = jnp.dot(direction, factor.astype(jnp.float32).T, precision=lax.Precision.HIGHEST)
    new_weight = old_weight - 0.05 * update
    near = copy_for_each(new_weight.astype(jnp.bfloat16), FS[1])
    copied = ring_gathered(near.reshape(-1, near.shape[-1]), FS[0])
    return (new_weight, update, new_first, new_second, copied.reshape(HV, -1))


def solution(mesh):
    finer = Mesh(mesh.devices.reshape(8, 8, mesh.shape["tp"]), (*FS, "tp"))
    in_specs = (P(FS, None), P(FS, "tp"), P(FS, "tp"), P("tp", None), P(FS, None), P(FS, None))
    out_specs = (P(FS, "tp"), P(FS, "tp"), P(FS, None), P(FS, None), P(None, "tp"))
    return jax.shard_map(
        on_device, mesh=finer, in_specs=in_specs, out_specs=out_specs, check_vma=False
    )
```

```python
import math

import jax
import jax.numpy as jnp
from jax import lax
from jax.experimental import pallas as pl
from jax.experimental.pallas import tpu as pltpu
from jax.sharding import Mesh
from jax.sharding import PartitionSpec as P

HV = 2048
RANK = 256
FS = ("fs_0", "fs_1")
TP = ("tp_0", "tp_1")
CHUNKS = 2


def exchanged(blocks, axis):
    return lax.all_to_all(blocks, axis, 0, 0, tiled=True)


def copy_for_each(shard, axis):
    devices = lax.axis_size(axis)
    return exchanged(jnp.broadcast_to(shard[None], (devices, *shard.shape)), axis)


def ring_gathered(shard, axis, lane):
    size, lanes = lax.axis_size(axis), lax.axis_size(lane)
    ways = [1 - 2 * (k % 2) for k in range(lanes)]
    hops = [
        (at * lanes + k, (at + ways[k]) % size * lanes + k)
        for at in range(size)
        for k in range(lanes)
    ]
    here = lax.axis_index(axis)
    way = 1 - 2 * (lax.axis_index(lane) % 2)
    rows = shard.shape[0] // CHUNKS
    whole = jnp.zeros((size, *shard.shape), shard.dtype)
    whole = lax.dynamic_update_slice(whole, shard[None], (here, 0, 0))
    chunks = [shard[k * rows : (k + 1) * rows] for k in range(CHUNKS)]
    for step in range(1, size):
        source = (here - way * step + size) % size
        for k in range(CHUNKS):
            chunks[k] = lax.ppermute(chunks[k], (axis, lane), hops)
            whole = lax.dynamic_update_slice(whole, chunks[k][None], (source, k * rows, 0))
    return whole


def projection_kernel(tp, rows, x_ref, g_ref, f_ref, o_ref, low_ref):
    step = pl.program_id(0)

    @pl.when(step == 0)
    def _():
        low = lax.dot_general(
            f_ref[...], g_ref[...], (((0,), (1,)), ((), ())), preferred_element_type=jnp.float32
        )
        high = low.astype(jnp.bfloat16)
        low_ref[:RANK] = high
        low_ref[RANK:] = (low - high.astype(jnp.float32)).astype(jnp.bfloat16)

    both = jnp.dot(low_ref[...], x_ref[...], preferred_element_type=jnp.float32)
    part = (both[:RANK] + both[RANK:]).astype(jnp.bfloat16)
    wide = x_ref.shape[1]
    held = wide // rows
    own = rows // tp
    to = lax.broadcasted_iota(jnp.int32, (wide, wide), 0)
    at = lax.broadcasted_iota(jnp.int32, (wide, wide), 1)
    source = to % (held * own) // own * rows + to // (held * own) * own + to % own
    turn = jnp.where(at == source, 1.0, 0.0).astype(jnp.bfloat16)
    turned = lax.dot_general(
        turn, part, (((1,), (1,)), ((), ())), preferred_element_type=jnp.float32
    )
    o_ref[...] = turned.astype(jnp.bfloat16).reshape(tp, held * own, RANK)


def projected_part(saved_input, out_cotangent, factor, fs, tp):
    tokens, wide = saved_input.shape
    width = out_cotangent.shape[1]
    rows = wide // fs
    step = 256
    held = step // tp
    kernel = lambda *refs: projection_kernel(tp, rows, *refs)
    return pl.pallas_call(
        kernel,
        grid=(wide // step,),
        in_specs=[
            pl.BlockSpec((tokens, step), lambda k: (0, k)),
            pl.BlockSpec((tokens, width), lambda k: (0, 0)),
            pl.BlockSpec((width, RANK), lambda k: (0, 0)),
        ],
        out_specs=pl.BlockSpec((tp, held, RANK), lambda k: (0, k, 0)),
        out_shape=jax.ShapeDtypeStruct((tp, wide // tp, RANK), jnp.bfloat16),
        scratch_shapes=[pltpu.VMEM((2 * RANK, tokens), jnp.bfloat16)],
        name="projection",
    )(saved_input, out_cotangent, factor)


def on_device(saved_input, out_cotangent, old_weight, factor, moment_first, moment_second):
    fs, tp = lax.axis_size(FS), lax.axis_size(TP)
    rows = HV // fs
    tiles = exchanged(projected_part(saved_input, out_cotangent, factor, fs, tp), TP)
    part = jnp.sum(tiles.astype(jnp.float32), axis=0).astype(jnp.bfloat16)
    tiles = exchanged(part.reshape(fs, rows // tp, RANK), FS)
    own = jnp.sum(tiles.astype(jnp.float32), axis=0)
    projected = copy_for_each(own, TP).reshape(rows, RANK)
    squares = jnp.full((1, 128), jnp.sum(projected * projected), jnp.float32)
    squares = jnp.sum(copy_for_each(squares, FS)[:, 0, 0])
    clip = jnp.minimum(1.0, math.sqrt(HV * RANK) / (jnp.sqrt(squares) + 1e-06))
    clipped = clip * projected
    new_first = 0.9 * moment_first + 0.1 * clipped
    new_second = 0.95 * moment_second + 0.05 * clipped * clipped
    direction = new_first / (jnp.sqrt(new_second) + 1e-08)
    update = jnp.dot(direction, factor.astype(jnp.float32).T, precision=lax.Precision.HIGHEST)
    new_weight = old_weight - 0.05 * update
    near = copy_for_each(new_weight.astype(jnp.bfloat16), FS[1])
    copied = ring_gathered(near.reshape(-1, near.shape[-1]), FS[0], TP[1])
    return (new_weight, update, new_first, new_second, copied.reshape(HV, -1))


def solution(mesh):
    finer = Mesh(mesh.devices.reshape(8, 8, mesh.shape["tp"] // 2, 2), (*FS, *TP))
    in_specs = (P(FS, None), P(FS, TP), P(FS, TP), P(TP, None), P(FS, None), P(FS, None))
    out_specs = (P(FS, TP), P(FS, TP), P(FS, None), P(FS, None), P(None, TP))
    return jax.shard_map(
        on_device, mesh=finer, in_specs=in_specs, out_specs=out_specs, check_vma=False
    )
```

```python
import math

import jax
import jax.numpy as jnp
from jax import lax
from jax.experimental import pallas as pl
from jax.sharding import Mesh
from jax.sharding import PartitionSpec as P

HV = 2048
RANK = 256
FS = ("fs_0", "fs_1")
LIMIT = math.sqrt(HV * RANK)


def exchanged(blocks, axis):
    return lax.all_to_all(blocks, axis, 0, 0, tiled=True)


def copy_for_each(shard, axis):
    devices = lax.axis_size(axis)
    return exchanged(jnp.broadcast_to(shard[None], (devices, *shard.shape)), axis)


def in_two(values):
    high = lax.reduce_precision(values, 8, 7)
    return high.astype(jnp.bfloat16), (values - high).astype(jnp.bfloat16)


def moments_after(clipped, first, second):
    return 0.9 * first + 0.1 * clipped, 0.95 * second + 0.05 * clipped * clipped


def copied_kernel(tp, rows, direction_ref, factor_ref, old_ref, o_ref):
    wide = old_ref.shape[0]
    own = rows // tp
    held = wide // rows * own
    at = lax.broadcasted_iota(jnp.int32, (wide, wide), 0)
    source = lax.broadcasted_iota(jnp.int32, (wide, wide), 1)
    wanted = at % rows // own * held + at // rows * own + at % own
    turn = jnp.where(source == wanted, 1.0, 0.0).astype(jnp.bfloat16)
    stacked = direction_ref[...].reshape(wide, RANK)
    direction = jnp.dot(turn, stacked, preferred_element_type=jnp.float32)
    update = lax.dot_general(
        direction.astype(jnp.bfloat16),
        factor_ref[...],
        (((1,), (1,)), ((), ())),
        preferred_element_type=jnp.float32,
    )
    o_ref[...] = (old_ref[...] - 0.05 * update).astype(jnp.bfloat16)


def copied_weight(directions, factor, old, fs, tp):
    hv, width = old.shape
    rows = hv // fs
    wide = 256
    held = wide // tp
    return pl.pallas_call(
        lambda *refs: copied_kernel(tp, rows, *refs),
        grid=(hv // wide,),
        in_specs=[
            pl.BlockSpec((tp, held, RANK), lambda k: (0, k, 0)),
            pl.BlockSpec((width, RANK), lambda k: (0, 0)),
            pl.BlockSpec((wide, width), lambda k: (k, 0)),
        ],
        out_specs=pl.BlockSpec((wide, width), lambda k: (k, 0)),
        out_shape=jax.ShapeDtypeStruct((hv, width), jnp.bfloat16),
        name="copied_weight",
    )(directions, factor, old)


def on_device(saved_input, out_cotangent, old_weight, factor, moment_first, moment_second):
    fs, tp = lax.axis_size(FS), lax.axis_size("tp")
    rows = HV // fs
    mine = rows // tp
    all_old = lax.all_gather(old_weight, FS, axis=0, tiled=True)
    contract = (((0,), (0,)), ((), ()))
    low = jnp.dot(out_cotangent, factor, preferred_element_type=jnp.float32)
    part = lax.dot_general(
        saved_input, low.astype(jnp.bfloat16), contract, preferred_element_type=jnp.float32
    )
    part = part.astype(jnp.bfloat16).reshape(fs, tp, mine, RANK).transpose(1, 0, 2, 3)
    tiles = exchanged(part.reshape(tp, fs * mine, RANK), "tp")
    part = jnp.sum(tiles.astype(jnp.float32), axis=0).reshape(fs, mine, RANK)
    own = jnp.sum(exchanged(part, FS), axis=0)

    start = lax.axis_index("tp") * mine
    own_first = lax.dynamic_slice(moment_first, (start, 0), (mine, RANK))
    own_second = lax.dynamic_slice(moment_second, (start, 0), (mine, RANK))
    sent = jnp.concatenate(
        [own.astype(jnp.bfloat16), *in_two(own_first), own_second.astype(jnp.bfloat16)]
    )
    held = copy_for_each(sent, FS).astype(jnp.float32)
    held = [held[:, k * mine : (k + 1) * mine] for k in range(4)]
    squares = jnp.full((1, RANK), jnp.sum(held[0] * held[0]), jnp.float32)
    sent = jnp.concatenate([own, squares, jnp.zeros((7 - mine, RANK), jnp.float32)])
    tiles = copy_for_each(sent, "tp")
    clip = jnp.minimum(1.0, LIMIT / (jnp.sqrt(jnp.sum(tiles[:, mine, 0])) + 1e-06))
    first, second = moments_after(clip * held[0], held[1] + held[2], held[3])
    directions = (first / (jnp.sqrt(second) + 1e-08)).astype(jnp.bfloat16)
    directions = copy_for_each(directions.reshape(fs * mine, RANK), "tp")

    projected = tiles[:, :mine].reshape(rows, RANK)
    new_first, new_second = moments_after(clip * projected, moment_first, moment_second)
    direction = new_first / (jnp.sqrt(new_second) + 1e-08)
    update = jnp.dot(direction, factor.astype(jnp.float32).T, precision=lax.Precision.HIGHEST)
    new_weight = old_weight - 0.05 * update
    copied = copied_weight(directions, factor, all_old, fs, tp)
    return (new_weight, update, new_first, new_second, copied)


def solution(mesh):
    finer = Mesh(mesh.devices.reshape(8, 8, mesh.shape["tp"]), (*FS, "tp"))
    in_specs = (P(FS, None), P(FS, "tp"), P(FS, "tp"), P("tp", None), P(FS, None), P(FS, None))
    out_specs = (P(FS, "tp"), P(FS, "tp"), P(FS, None), P(FS, None), P(None, "tp"))
    return jax.shard_map(
        on_device, mesh=finer, in_specs=in_specs, out_specs=out_specs, check_vma=False
    )
```

```python
import math

import jax
import jax.numpy as jnp
from jax import lax
from jax.sharding import Mesh
from jax.sharding import PartitionSpec as P

HV = 2048
RANK = 256
FS = ("fs_0", "fs_1")


def exchanged(blocks, axis):
    return lax.all_to_all(blocks, axis, 0, 0, tiled=True)


def copy_for_each(shard, axis):
    devices = lax.axis_size(axis)
    return exchanged(jnp.broadcast_to(shard[None], (devices, *shard.shape)), axis)


def ring_gathered(shard, axis):
    size = lax.axis_size(axis)
    here = lax.axis_index(axis)
    way = 1 - 2 * (here % 2)
    pairs = [[(k, k ^ 1) for k in range(size)]]
    pairs.append([(k, ((k + 1) ^ 1) - 1) for k in range(size)])
    pairs[1] = [(k, to % size) for k, to in pairs[1]]
    half = shard.shape[0] // 2
    whole = jnp.zeros((size, *shard.shape), shard.dtype)

    def put(whole, block, at, row=0):
        return lax.dynamic_update_slice(whole, block[None], ((at + size) % size, row, 0))

    whole = put(whole, shard, here)
    first = second = shard
    for step in range(1, size // 2):
        second, first = (
            lax.ppermute(first, axis, pairs[0]),
            lax.ppermute(second, axis, pairs[1]),
        )
        whole = put(whole, second, here + way * step)
        whole = put(whole, first, here - way * step)
    far = here + size // 2
    whole = put(whole, lax.ppermute(first[:half], axis, pairs[0]), far)
    return put(whole, lax.ppermute(second[half:], axis, pairs[1]), far, half)


def on_device(saved_input, out_cotangent, old_weight, factor, moment_first, moment_second):
    fs, tp = lax.axis_size(FS), lax.axis_size("tp")
    rows = HV // fs
    contract = (((0,), (0,)), ((), ()))
    low = jnp.dot(out_cotangent, factor, preferred_element_type=jnp.float32)
    part = lax.dot_general(
        saved_input, low.astype(jnp.bfloat16), contract, preferred_element_type=jnp.float32
    )
    part = part.astype(jnp.bfloat16).reshape(fs, tp, rows // tp, RANK).transpose(1, 0, 2, 3)
    tiles = exchanged(part.reshape(tp, fs * rows // tp, RANK), "tp")
    part = jnp.sum(tiles.astype(jnp.float32), axis=0).reshape(fs, rows // tp, RANK)
    own = jnp.sum(exchanged(part, FS), axis=0)
    projected = copy_for_each(own, "tp").reshape(rows, RANK)
    squares = jnp.full((1, 128), jnp.sum(projected * projected), jnp.float32)
    squares = jnp.sum(copy_for_each(squares, FS)[:, 0, 0])
    clip = jnp.minimum(1.0, math.sqrt(HV * RANK) / (jnp.sqrt(squares) + 1e-06))
    clipped = clip * projected
    new_first = 0.9 * moment_first + 0.1 * clipped
    new_second = 0.95 * moment_second + 0.05 * clipped * clipped
    direction = new_first / (jnp.sqrt(new_second) + 1e-08)
    update = jnp.dot(direction, factor.astype(jnp.float32).T, precision=lax.Precision.HIGHEST)
    new_weight = old_weight - 0.05 * update
    near = copy_for_each(new_weight.astype(jnp.bfloat16), FS[1])
    copied = ring_gathered(near.reshape(-1, near.shape[-1]), FS[0])
    return (new_weight, update, new_first, new_second, copied.reshape(HV, -1))


def solution(mesh):
    finer = Mesh(mesh.devices.reshape(8, 8, mesh.shape["tp"]), (*FS, "tp"))
    in_specs = (P(FS, None), P(FS, "tp"), P(FS, "tp"), P("tp", None), P(FS, None), P(FS, None))
    out_specs = (P(FS, "tp"), P(FS, "tp"), P(FS, None), P(FS, None), P(None, "tp"))
    return jax.shard_map(
        on_device, mesh=finer, in_specs=in_specs, out_specs=out_specs, check_vma=False
    )
```

```python
import math

import jax
import jax.numpy as jnp
import numpy as np
from jax import lax
from jax.experimental import pallas as pl
from jax.experimental.pallas import tpu as pltpu
from jax.sharding import Mesh
from jax.sharding import PartitionSpec as P

HV = 2048
RANK = 256
FS = ("fs_0", "fs_1")
LIMIT = math.sqrt(HV * RANK)


def exchanged(blocks, axis):
    return lax.all_to_all(blocks, axis, 0, 0, tiled=True)


def copy_for_each(shard, axis):
    devices = lax.axis_size(axis)
    return exchanged(jnp.broadcast_to(shard[None], (devices, *shard.shape)), axis)


def shifted(shard, axis, by):
    size = lax.axis_size(axis)
    return lax.ppermute(shard, axis, [(k, (k + by) % size) for k in range(size)])


def ring_gathered(shard, axis):
    size = lax.axis_size(axis)
    here = lax.axis_index(axis)
    half = shard.shape[0] // 2
    whole = jnp.zeros((shard.shape[0], size, *shard.shape[1:]), shard.dtype)

    def put(whole, block, at, row=0):
        at = (at + size) % size
        return lax.dynamic_update_slice(whole, block[:, None], (row, at, 0, 0))

    whole = put(whole, shard, here)
    up = down = shard
    for step in range(1, size // 2):
        up, down = shifted(up, axis, 1), shifted(down, axis, -1)
        whole = put(whole, up, here - step)
        whole = put(whole, down, here + step)
    far = here + size // 2
    whole = put(whole, shifted(up[:half], axis, 1), far)
    return put(whole, shifted(down[half:], axis, -1), far, half)


def projection_kernel(x_ref, g_ref, f_ref, turn_ref, o_ref, low_ref):
    @pl.when(pl.program_id(0) == 0)
    def _():
        low = lax.dot_general(
            f_ref[...], g_ref[...], (((0,), (1,)), ((), ())), preferred_element_type=jnp.float32
        )
        high = low.astype(jnp.bfloat16)
        low_ref[:RANK] = high
        low_ref[RANK:] = (low - high.astype(jnp.float32)).astype(jnp.bfloat16)

    both = jnp.dot(low_ref[...], x_ref[...], preferred_element_type=jnp.float32)
    part = (both[:RANK] + both[RANK:]).astype(jnp.bfloat16)
    turned = lax.dot_general(
        turn_ref[...], part, (((1,), (1,)), ((), ())), preferred_element_type=jnp.float32
    )
    o_ref[...] = turned.astype(jnp.bfloat16).reshape(o_ref.shape)


def projected_part(saved_input, out_cotangent, factor, fs, tp):
    tokens, wide = saved_input.shape
    width = out_cotangent.shape[1]
    step = 256
    held = step // tp
    order = np.arange(step).reshape(step * fs // wide, tp, -1).transpose(1, 0, 2).reshape(-1)
    turn = jnp.asarray(np.eye(step, dtype=np.float32)[order], jnp.bfloat16)
    return pl.pallas_call(
        projection_kernel,
        grid=(wide // step,),
        in_specs=[
            pl.BlockSpec((tokens, step), lambda k: (0, k)),
            pl.BlockSpec((tokens, width), lambda k: (0, 0)),
            pl.BlockSpec((width, RANK), lambda k: (0, 0)),
            pl.BlockSpec((step, step), lambda k: (0, 0)),
        ],
        out_specs=pl.BlockSpec((tp, held, RANK), lambda k: (0, k, 0)),
        out_shape=jax.ShapeDtypeStruct((tp, wide // tp, RANK), jnp.bfloat16),
        scratch_shapes=[pltpu.VMEM((2 * RANK, tokens), jnp.bfloat16)],
        name="projection",
    )(saved_input, out_cotangent, factor, turn)


def on_device(saved_input, out_cotangent, old_weight, factor, moment_first, moment_second):
    fs, tp = lax.axis_size(FS), lax.axis_size("tp")
    rows = HV // fs
    tiles = exchanged(projected_part(saved_input, out_cotangent, factor, fs, tp), "tp")
    part = jnp.sum(tiles.astype(jnp.float32), axis=0).astype(jnp.bfloat16)
    tiles = exchanged(part.reshape(fs, rows // tp, RANK), FS)
    own = jnp.sum(tiles.astype(jnp.float32), axis=0)
    projected = lax.optimization_barrier(copy_for_each(own, "tp").reshape(rows, RANK))
    squares = jnp.sum(projected * projected, axis=0, keepdims=True)
    squares = jnp.sum(copy_for_each(squares, FS), axis=0)
    ones = jnp.ones((RANK, RANK), jnp.float32)
    squares = jnp.dot(squares, ones, precision=lax.Precision.HIGHEST)
    clip = jnp.minimum(1.0, LIMIT / (jnp.sqrt(squares) + 1e-06))
    clipped = clip * projected
    new_first = 0.9 * moment_first + 0.1 * clipped
    new_second = 0.95 * moment_second + 0.05 * clipped * clipped
    direction = new_first / (jnp.sqrt(new_second) + 1e-08)
    update = jnp.dot(direction, factor.astype(jnp.float32).T, precision=lax.Precision.HIGHEST)
    new_weight = old_weight - 0.05 * update
    near = copy_for_each(new_weight.astype(jnp.bfloat16), FS[0])
    copied = ring_gathered(near, FS[1])
    return (new_weight, update, new_first, new_second, copied.reshape(HV, -1))


def solution(mesh):
    finer = Mesh(mesh.devices.reshape(8, 8, mesh.shape["tp"]), (*FS, "tp"))
    in_specs = (P(FS, None), P(FS, "tp"), P(FS, "tp"), P("tp", None), P(FS, None), P(FS, None))
    out_specs = (P(FS, "tp"), P(FS, "tp"), P(FS, None), P(FS, None), P(None, "tp"))
    return jax.shard_map(
        on_device, mesh=finer, in_specs=in_specs, out_specs=out_specs, check_vma=False
    )
```

```python
import math

import jax
import jax.numpy as jnp
from jax import lax
from jax.sharding import Mesh
from jax.sharding import PartitionSpec as P

HV = 2048
RANK = 256
FS = ("fs_0", "fs_1")


def exchanged(blocks, axis):
    return lax.all_to_all(blocks, axis, 0, 0, tiled=True)


def copy_for_each(shard, axis):
    devices = lax.axis_size(axis)
    return exchanged(jnp.broadcast_to(shard[None], (devices, *shard.shape)), axis)


def shifted(shard, axis, by):
    size = lax.axis_size(axis)
    return lax.ppermute(shard, axis, [(k, (k + by) % size) for k in range(size)])


def ring_gathered(shard, axis):
    size = lax.axis_size(axis)
    here = lax.axis_index(axis)
    half = shard.shape[0] // 2
    whole = jnp.zeros((size, *shard.shape), shard.dtype)

    def put(whole, block, at, row=0):
        return lax.dynamic_update_slice(whole, block[None], (at % size, row, 0))

    whole = put(whole, shard, here)
    up = down = shard
    for step in range(1, size // 2):
        up, down = shifted(up, axis, 1), shifted(down, axis, -1)
        whole = put(whole, up, here - step + size)
        whole = put(whole, down, here + step)
    far = here + size // 2
    whole = put(whole, shifted(up[:half], axis, 1), far)
    whole = put(whole, shifted(down[half:], axis, -1), far, half)
    return whole.reshape(-1, *shard.shape[1:])


def on_device(saved_input, out_cotangent, old_weight, factor, moment_first, moment_second):
    fs, tp = lax.axis_size(FS), lax.axis_size("tp")
    rows = HV // fs
    width = old_weight.shape[1]
    held = jnp.concatenate([old_weight, moment_first, moment_second], axis=1)
    held = ring_gathered(held, FS[1])
    old, first, second = jnp.split(held, [width, width + RANK], axis=1)

    contract = (((0,), (0,)), ((), ()))
    low = jnp.dot(out_cotangent, factor, preferred_element_type=jnp.float32)
    part = lax.dot_general(
        saved_input, low.astype(jnp.bfloat16), contract, preferred_element_type=jnp.float32
    )
    part = part.astype(jnp.bfloat16).reshape(fs, tp, rows // tp, RANK).transpose(1, 0, 2, 3)
    tiles = exchanged(part.reshape(tp, fs * rows // tp, RANK), "tp")
    part = jnp.sum(tiles.astype(jnp.float32), axis=0).reshape(fs, rows // tp, RANK)
    own = jnp.sum(exchanged(part, FS), axis=0)

    projected = lax.optimization_barrier(copy_for_each(own, (FS[1], "tp")).reshape(-1, RANK))
    squares = jnp.sum(projected * projected, axis=0, keepdims=True)
    squares = jnp.sum(copy_for_each(squares, FS[0]), axis=0)
    ones = jnp.ones((RANK, RANK), jnp.float32)
    squares = jnp.dot(squares, ones, precision=lax.Precision.HIGHEST)
    clip = jnp.minimum(1.0, math.sqrt(HV * RANK) / (jnp.sqrt(squares) + 1e-06))
    clipped = clip * projected
    first = 0.9 * first + 0.1 * clipped
    second = 0.95 * second + 0.05 * clipped * clipped
    direction = first / (jnp.sqrt(second) + 1e-08)
    update = jnp.dot(direction, factor.astype(jnp.float32).T, precision=lax.Precision.HIGHEST)
    weight = old - 0.05 * update
    copied = ring_gathered(weight.astype(jnp.bfloat16), FS[0])
    here = lax.axis_index(FS[1]) * rows
    mine = [lax.dynamic_slice_in_dim(x, here, rows) for x in (weight, update, first, second)]
    return (*mine, copied)


def solution(mesh):
    finer = Mesh(mesh.devices.reshape(8, 8, mesh.shape["tp"]), (*FS, "tp"))
    in_specs = (P(FS, None), P(FS, "tp"), P(FS, "tp"), P("tp", None), P(FS, None), P(FS, None))
    out_specs = (P(FS, "tp"), P(FS, "tp"), P(FS, None), P(FS, None), P(None, "tp"))
    return jax.shard_map(
        on_device, mesh=finer, in_specs=in_specs, out_specs=out_specs, check_vma=False
    )
```

```python
import math

import jax
import jax.numpy as jnp
from jax import lax
from jax.sharding import Mesh
from jax.sharding import PartitionSpec as P

HV = 2048
RANK = 256
FS = ("fs_0", "fs_1")
LIMIT = math.sqrt(HV * RANK)


def exchanged(blocks, axis):
    return lax.all_to_all(blocks, axis, 0, 0, tiled=True)


def copy_for_each(shard, axis):
    devices = lax.axis_size(axis)
    return exchanged(jnp.broadcast_to(shard[None], (devices, *shard.shape)), axis)


def in_two(values):
    high = lax.reduce_precision(values, 8, 7)
    return high.astype(jnp.bfloat16), (values - high).astype(jnp.bfloat16)


def moments_after(clipped, first, second):
    return 0.9 * first + 0.1 * clipped, 0.95 * second + 0.05 * clipped * clipped


def on_device(saved_input, out_cotangent, old_weight, factor, moment_first, moment_second):
    fs, tp = lax.axis_size(FS), lax.axis_size("tp")
    rows = HV // fs
    mine = rows // tp
    all_old = lax.all_gather(old_weight, FS, axis=0, tiled=True)
    contract = (((0,), (0,)), ((), ()))
    low = jnp.dot(out_cotangent, factor, preferred_element_type=jnp.float32)
    part = lax.dot_general(
        saved_input, low.astype(jnp.bfloat16), contract, preferred_element_type=jnp.float32
    )
    part = part.astype(jnp.bfloat16).reshape(fs, tp, mine, RANK).transpose(1, 0, 2, 3)
    start = lax.axis_index("tp") * mine
    own_first = lax.dynamic_slice(moment_first, (start, 0), (mine, RANK))
    own_second = lax.dynamic_slice(moment_second, (start, 0), (mine, RANK))
    moments = jnp.concatenate([*in_two(own_first), own_second.astype(jnp.bfloat16)])
    part, moments = lax.optimization_barrier((part.reshape(tp, fs * mine, RANK), moments))
    tiles = exchanged(part, "tp")
    part = jnp.sum(tiles.astype(jnp.float32), axis=0).astype(jnp.bfloat16)
    tiles = exchanged(part.reshape(fs, mine, RANK), FS)
    own = jnp.sum(tiles.astype(jnp.float32), axis=0)

    held = copy_for_each(jnp.concatenate([own.astype(jnp.bfloat16), moments]), FS)
    held = lax.optimization_barrier(held.astype(jnp.float32))
    held = [held[:, k * mine : (k + 1) * mine] for k in range(4)]
    squares = jnp.sum(held[0] * held[0], axis=(0, 1))[None]
    sent = jnp.concatenate([own, jnp.broadcast_to(squares, (8 - mine, RANK))])
    tiles = copy_for_each(sent, "tp")
    squares = jnp.sum(tiles[:, mine], axis=0, keepdims=True)
    ones = jnp.ones((RANK, RANK), jnp.float32)
    squares = jnp.dot(squares, ones, precision=lax.Precision.HIGHEST)
    clip = jnp.minimum(1.0, LIMIT / (jnp.sqrt(squares) + 1e-06))
    first, second = moments_after(clip * held[0], held[1] + held[2], held[3])
    directions = (first / (jnp.sqrt(second) + 1e-08)).astype(jnp.bfloat16)
    directions = copy_for_each(directions.reshape(fs * mine, RANK), "tp")

    directions, tiles, clip = lax.optimization_barrier((directions, tiles, clip))
    directions = directions.reshape(tp, fs, mine, RANK).transpose(1, 0, 2, 3).reshape(HV, RANK)
    copied = lax.dot_general(
        directions, factor, (((1,), (1,)), ((), ())), preferred_element_type=jnp.float32
    )
    copied = (all_old - 0.05 * copied).astype(jnp.bfloat16)
    projected = tiles[:, :mine].reshape(rows, RANK)
    new_first, new_second = moments_after(clip * projected, moment_first, moment_second)
    direction = new_first / (jnp.sqrt(new_second) + 1e-08)
    update = jnp.dot(direction, factor.astype(jnp.float32).T, precision=lax.Precision.HIGHEST)
    new_weight = old_weight - 0.05 * update
    return (new_weight, update, new_first, new_second, copied)


def solution(mesh):
    finer = Mesh(mesh.devices.reshape(8, 8, mesh.shape["tp"]), (*FS, "tp"))
    in_specs = (P(FS, None), P(FS, "tp"), P(FS, "tp"), P("tp", None), P(FS, None), P(FS, None))
    out_specs = (P(FS, "tp"), P(FS, "tp"), P(FS, None), P(FS, None), P(None, "tp"))
    return jax.shard_map(
        on_device, mesh=finer, in_specs=in_specs, out_specs=out_specs, check_vma=False
    )
```

```python
import math

import jax
import jax.numpy as jnp
from jax import lax
from jax.sharding import Mesh
from jax.sharding import PartitionSpec as P

HV = 2048
RANK = 256
FS = ("fs_0", "fs_1")
TP = ("tp_0", "tp_1")
LIMIT = math.sqrt(HV * RANK)


def exchanged(blocks, axis):
    return lax.all_to_all(blocks, axis, 0, 0, tiled=True)


def copy_for_each(shard, axis):
    devices = lax.axis_size(axis)
    return exchanged(jnp.broadcast_to(shard[None], (devices, *shard.shape)), axis)


def in_two(values):
    high = lax.reduce_precision(values, 8, 7)
    return high.astype(jnp.bfloat16), (values - high).astype(jnp.bfloat16)


def moments_after(clipped, first, second):
    return 0.9 * first + 0.1 * clipped, 0.95 * second + 0.05 * clipped * clipped


def on_device(saved_input, out_cotangent, old_weight, factor, moment_first, moment_second):
    fs, tp = lax.axis_size(FS), lax.axis_size(TP)
    rows = HV // fs
    mine = rows // tp
    all_old = lax.all_gather(old_weight, FS, axis=0, tiled=True)
    contract = (((0,), (0,)), ((), ()))
    low = jnp.dot(out_cotangent, factor, preferred_element_type=jnp.float32)
    part = lax.dot_general(
        saved_input, low.astype(jnp.bfloat16), contract, preferred_element_type=jnp.float32
    )
    part = part.astype(jnp.bfloat16).reshape(fs, tp, mine, RANK).transpose(1, 0, 2, 3)
    start = (lax.axis_index(TP) * mine).astype(jnp.uint32)
    part, start = lax.optimization_barrier((part.reshape(tp, fs * mine, RANK), start))
    tiles = exchanged(part, TP)
    part = jnp.sum(tiles.astype(jnp.float32), axis=0).astype(jnp.bfloat16)
    tiles = exchanged(part.reshape(fs, mine, RANK), FS)
    own = jnp.sum(tiles.astype(jnp.float32), axis=0)

    own, first, second = lax.optimization_barrier((own, moment_first, moment_second))
    own_first = lax.dynamic_slice(first, (start, jnp.uint32(0)), (mine, RANK))
    own_second = lax.dynamic_slice(second, (start, jnp.uint32(0)), (mine, RANK))
    moments = [*in_two(own_first), own_second.astype(jnp.bfloat16)]
    held = copy_for_each(jnp.concatenate([own.astype(jnp.bfloat16), *moments]), FS)
    held = lax.optimization_barrier(held.astype(jnp.float32))
    held = [held[:, k * mine : (k + 1) * mine] for k in range(4)]
    squares = jnp.sum(held[0] * held[0], axis=(0, 1))[None]
    sent = jnp.concatenate([own, jnp.broadcast_to(squares, (8 - mine, RANK))])
    tiles = copy_for_each(sent, TP)
    squares = jnp.sum(tiles[:, mine], axis=0, keepdims=True)
    ones = jnp.ones((RANK, RANK), jnp.float32)
    squares = jnp.dot(squares, ones, precision=lax.Precision.HIGHEST)
    clip = jnp.minimum(1.0, LIMIT / (jnp.sqrt(squares) + 1e-06))
    all_first, all_second = moments_after(clip * held[0], held[1] + held[2], held[3])
    directions = (all_first / (jnp.sqrt(all_second) + 1e-08)).astype(jnp.bfloat16)
    directions = copy_for_each(directions.reshape(fs * mine, RANK), TP[0])
    directions, all_old = lax.optimization_barrier((directions, all_old))
    directions = copy_for_each(directions.reshape(-1, RANK), TP[1])

    directions, tiles, clip = lax.optimization_barrier((directions, tiles, clip))
    projected = tiles[:, :mine].reshape(rows, RANK)
    new_first, new_second = moments_after(clip * projected, first, second)
    direction = new_first / (jnp.sqrt(new_second) + 1e-08)
    update = jnp.dot(direction, factor.astype(jnp.float32).T, precision=lax.Precision.HIGHEST)
    new_weight = old_weight - 0.05 * update
    mine = (new_weight, update, new_first, new_second)
    directions, mine = lax.optimization_barrier((directions, mine))
    directions = directions.reshape(lax.axis_size(TP[1]), lax.axis_size(TP[0]), fs, rows // tp, RANK)
    directions = directions.transpose(2, 1, 0, 3, 4).reshape(HV, RANK)
    copied = lax.dot_general(
        directions, factor, (((1,), (1,)), ((), ())), preferred_element_type=jnp.float32
    )
    copied = (all_old - 0.05 * copied).astype(jnp.bfloat16)
    return (*mine, copied)


def solution(mesh):
    finer = Mesh(mesh.devices.reshape(8, 8, mesh.shape["tp"] // 2, 2), (*FS, *TP))
    in_specs = (P(FS, None), P(FS, TP), P(FS, TP), P(TP, None), P(FS, None), P(FS, None))
    out_specs = (P(FS, TP), P(FS, TP), P(FS, None), P(FS, None), P(None, TP))
    return jax.shard_map(
        on_device, mesh=finer, in_specs=in_specs, out_specs=out_specs, check_vma=False
    )
```

```python
import math

import jax
import jax.numpy as jnp
import numpy as np
from jax import lax
from jax.experimental import pallas as pl
from jax.experimental.pallas import tpu as pltpu
from jax.sharding import Mesh
from jax.sharding import PartitionSpec as P

HV = 2048
RANK = 256
FS = ("fs_0", "fs_1")
TP = ("tp_0", "tp_1")
LIMIT = math.sqrt(HV * RANK)


def exchanged(blocks, axis):
    return lax.all_to_all(blocks, axis, 0, 0, tiled=True)


def copy_for_each(shard, axis):
    devices = lax.axis_size(axis)
    return exchanged(jnp.broadcast_to(shard[None], (devices, *shard.shape)), axis)


def in_two(values):
    high = lax.reduce_precision(values, 8, 7)
    return high.astype(jnp.bfloat16), (values - high).astype(jnp.bfloat16)


def moments_after(clipped, first, second):
    return 0.9 * first + 0.1 * clipped, 0.95 * second + 0.05 * clipped * clipped


def projection_kernel(held, x_ref, g_ref, f_ref, turn_ref, o_ref, low_ref):
    @pl.when(pl.program_id(0) == 0)
    def _():
        low = lax.dot_general(
            f_ref[...], g_ref[...], (((0,), (1,)), ((), ())), preferred_element_type=jnp.float32
        )
        high = low.astype(jnp.bfloat16)
        low_ref[:RANK] = high
        low_ref[RANK:] = (low - high.astype(jnp.float32)).astype(jnp.bfloat16)

    both = jnp.dot(low_ref[...], x_ref[...], preferred_element_type=jnp.float32)
    part = (both[:RANK] + both[RANK:]).astype(jnp.bfloat16)
    wide = turn_ref.shape[0]
    for k in range(part.shape[1] // wide):
        turned = lax.dot_general(
            turn_ref[...],
            part[:, k * wide : (k + 1) * wide],
            (((1,), (1,)), ((), ())),
            preferred_element_type=jnp.float32,
        )
        turned = turned.astype(jnp.bfloat16).reshape(-1, held, RANK)
        o_ref[:, k * held : (k + 1) * held] = turned


def projected_part(saved_input, out_cotangent, factor, fs, tp):
    tokens, wide = saved_input.shape
    width = out_cotangent.shape[1]
    step, turned = 1024, 256
    order = np.arange(turned).reshape(turned * fs // wide, tp, -1).transpose(1, 0, 2).reshape(-1)
    turn = jnp.asarray(np.eye(turned, dtype=np.float32)[order], jnp.bfloat16)
    return pl.pallas_call(
        lambda *refs: projection_kernel(turned // tp, *refs),
        grid=(wide // step,),
        in_specs=[
            pl.BlockSpec((tokens, step), lambda k: (0, k)),
            pl.BlockSpec((tokens, width), lambda k: (0, 0)),
            pl.BlockSpec((width, RANK), lambda k: (0, 0)),
            pl.BlockSpec((turned, turned), lambda k: (0, 0)),
        ],
        out_specs=pl.BlockSpec((tp, step // tp, RANK), lambda k: (0, k, 0)),
        out_shape=jax.ShapeDtypeStruct((tp, wide // tp, RANK), jnp.bfloat16),
        scratch_shapes=[pltpu.VMEM((2 * RANK, tokens), jnp.bfloat16)],
        name="projection",
    )(saved_input, out_cotangent, factor, turn)


def on_device(saved_input, out_cotangent, old_weight, factor, moment_first, moment_second):
    fs, tp = lax.axis_size(FS), lax.axis_size(TP)
    rows = HV // fs
    mine = rows // tp
    all_old = lax.all_gather(old_weight, FS, axis=0, tiled=True)
    part = projected_part(saved_input, out_cotangent, factor, fs, tp)
    start = (lax.axis_index(TP) * mine).astype(jnp.uint32)
    part, start = lax.optimization_barrier((part, start))
    tiles = exchanged(part, TP)
    part = jnp.sum(tiles.astype(jnp.float32), axis=0).astype(jnp.bfloat16)
    tiles = exchanged(part.reshape(fs, mine, RANK), FS)
    own = jnp.sum(tiles.astype(jnp.float32), axis=0)

    own, first, second = lax.optimization_barrier((own, moment_first, moment_second))
    own_first = lax.dynamic_slice(first, (start, jnp.uint32(0)), (mine, RANK))
    own_second = lax.dynamic_slice(second, (start, jnp.uint32(0)), (mine, RANK))
    moments = [*in_two(own_first), own_second.astype(jnp.bfloat16)]
    held = copy_for_each(jnp.concatenate([own.astype(jnp.bfloat16), *moments]), FS)
    held = lax.optimization_barrier(held.astype(jnp.float32))
    held = [held[:, k * mine : (k + 1) * mine] for k in range(4)]
    squares = jnp.sum(held[0] * held[0], axis=(0, 1))[None]
    sent = jnp.concatenate([own, jnp.broadcast_to(squares, (8 - mine, RANK))])
    tiles = copy_for_each(sent, TP)
    squares = jnp.sum(tiles[:, mine], axis=0, keepdims=True)
    ones = jnp.ones((RANK, RANK), jnp.float32)
    squares = jnp.dot(squares, ones, precision=lax.Precision.HIGHEST)
    clip = jnp.minimum(1.0, LIMIT / (jnp.sqrt(squares) + 1e-06))
    all_first, all_second = moments_after(clip * held[0], held[1] + held[2], held[3])
    directions = (all_first / (jnp.sqrt(all_second) + 1e-08)).astype(jnp.bfloat16)
    directions = copy_for_each(directions, TP[0])
    directions, all_old = lax.optimization_barrier((directions, all_old))
    directions = copy_for_each(directions, TP[1])

    directions, tiles, clip = lax.optimization_barrier((directions, tiles, clip))
    projected = tiles[:, :mine].reshape(rows, RANK)
    new_first, new_second = moments_after(clip * projected, first, second)
    direction = new_first / (jnp.sqrt(new_second) + 1e-08)
    update = jnp.dot(direction, factor.astype(jnp.float32).T, precision=lax.Precision.HIGHEST)
    new_weight = old_weight - 0.05 * update
    mine = (new_weight, update, new_first, new_second)
    directions, mine = lax.optimization_barrier((directions, mine))
    directions = directions.transpose(2, 1, 0, 3, 4).reshape(HV, RANK)
    copied = lax.dot_general(
        directions, factor, (((1,), (1,)), ((), ())), preferred_element_type=jnp.float32
    )
    copied = (all_old - 0.05 * copied).astype(jnp.bfloat16)
    return (*mine, copied)


def solution(mesh):
    finer = Mesh(mesh.devices.reshape(8, 8, mesh.shape["tp"] // 2, 2), (*FS, *TP))
    in_specs = (P(FS, None), P(FS, TP), P(FS, TP), P(TP, None), P(FS, None), P(FS, None))
    out_specs = (P(FS, TP), P(FS, TP), P(FS, None), P(FS, None), P(None, TP))
    return jax.shard_map(
        on_device, mesh=finer, in_specs=in_specs, out_specs=out_specs, check_vma=False
    )
```

```python
import math

import jax
import jax.numpy as jnp
import numpy as np
from jax import lax
from jax.experimental import pallas as pl
from jax.experimental.pallas import tpu as pltpu
from jax.sharding import Mesh
from jax.sharding import PartitionSpec as P

HV = 2048
RANK = 256
FS = ("fs_0", "fs_1")
TP = ("tp_0", "tp_1")
LIMIT = math.sqrt(HV * RANK)


def exchanged(blocks, axis):
    return lax.all_to_all(blocks, axis, 0, 0, tiled=True)


def copy_for_each(shard, axis):
    devices = lax.axis_size(axis)
    return exchanged(jnp.broadcast_to(shard[None], (devices, *shard.shape)), axis)


def in_two(values):
    high = lax.reduce_precision(values, 8, 7)
    return high.astype(jnp.bfloat16), (values - high).astype(jnp.bfloat16)


def moments_after(clipped, first, second):
    return 0.9 * first + 0.1 * clipped, 0.95 * second + 0.05 * clipped * clipped


def projection_kernel(held, x_ref, g_ref, f_ref, turn_ref, o_ref, low_ref):
    @pl.when(pl.program_id(0) == 0)
    def _():
        low = lax.dot_general(
            f_ref[...], g_ref[...], (((0,), (1,)), ((), ())), preferred_element_type=jnp.float32
        )
        high = low.astype(jnp.bfloat16)
        low_ref[:RANK] = high
        low_ref[RANK:] = (low - high.astype(jnp.float32)).astype(jnp.bfloat16)

    both = jnp.dot(low_ref[...], x_ref[...], preferred_element_type=jnp.float32)
    part = (both[:RANK] + both[RANK:]).astype(jnp.bfloat16)
    wide = turn_ref.shape[0]
    for k in range(part.shape[1] // wide):
        turned = lax.dot_general(
            turn_ref[...],
            part[:, k * wide : (k + 1) * wide],
            (((1,), (1,)), ((), ())),
            preferred_element_type=jnp.float32,
        )
        turned = turned.astype(jnp.bfloat16).reshape(-1, held, RANK)
        o_ref[:, k * held : (k + 1) * held] = turned


def projected_part(saved_input, out_cotangent, factor, fs, tp):
    tokens, wide = saved_input.shape
    width = out_cotangent.shape[1]
    step, turned = 1024, 256
    lanes = lax.axis_size(TP[1])
    order = np.arange(turned).reshape(turned * fs // wide, tp // lanes, lanes, -1)
    order = order.transpose(2, 1, 0, 3).reshape(-1)
    turn = jnp.asarray(np.eye(turned, dtype=np.float32)[order], jnp.bfloat16)
    return pl.pallas_call(
        lambda *refs: projection_kernel(turned // tp, *refs),
        grid=(wide // step,),
        in_specs=[
            pl.BlockSpec((tokens, step), lambda k: (0, k)),
            pl.BlockSpec((tokens, width), lambda k: (0, 0)),
            pl.BlockSpec((width, RANK), lambda k: (0, 0)),
            pl.BlockSpec((turned, turned), lambda k: (0, 0)),
        ],
        out_specs=pl.BlockSpec((tp, step // tp, RANK), lambda k: (0, k, 0)),
        out_shape=jax.ShapeDtypeStruct((tp, wide // tp, RANK), jnp.bfloat16),
        scratch_shapes=[pltpu.VMEM((2 * RANK, tokens), jnp.bfloat16)],
        name="projection",
    )(saved_input, out_cotangent, factor, turn)


def on_device(saved_input, out_cotangent, old_weight, factor, moment_first, moment_second):
    fs, tp = lax.axis_size(FS), lax.axis_size(TP)
    rows = HV // fs
    mine = rows // tp
    all_old = lax.all_gather(old_weight, FS, axis=0, tiled=True)
    part = projected_part(saved_input, out_cotangent, factor, fs, tp)
    start = (lax.axis_index(TP) * mine).astype(jnp.uint32)
    part, start = lax.optimization_barrier((part, start))
    for axis in reversed(TP):
        devices = lax.axis_size(axis)
        tiles = exchanged(part.reshape(devices, -1, RANK), axis)
        part = jnp.sum(tiles.astype(jnp.float32), axis=0).astype(jnp.bfloat16)
    tiles = exchanged(part.reshape(fs, mine, RANK), FS)
    own = jnp.sum(tiles.astype(jnp.float32), axis=0)

    own, first, second = lax.optimization_barrier((own, moment_first, moment_second))
    own_first = lax.dynamic_slice(first, (start, jnp.uint32(0)), (mine, RANK))
    own_second = lax.dynamic_slice(second, (start, jnp.uint32(0)), (mine, RANK))
    moments = [*in_two(own_first), own_second.astype(jnp.bfloat16)]
    held = copy_for_each(jnp.concatenate([own.astype(jnp.bfloat16), *moments]), FS)
    held = lax.optimization_barrier(held.astype(jnp.float32))
    held = [held[:, k * mine : (k + 1) * mine] for k in range(4)]
    squares = jnp.sum(held[0] * held[0], axis=(0, 1))[None]
    sent = jnp.concatenate([own, jnp.broadcast_to(squares, (8 - mine, RANK))])
    tiles = copy_for_each(sent, TP)
    squares = jnp.sum(tiles[:, mine], axis=0, keepdims=True)
    ones = jnp.ones((RANK, RANK), jnp.float32)
    squares = jnp.dot(squares, ones, precision=lax.Precision.HIGHEST)
    clip = jnp.minimum(1.0, LIMIT / (jnp.sqrt(squares) + 1e-06))
    all_first, all_second = moments_after(clip * held[0], held[1] + held[2], held[3])
    directions = (all_first / (jnp.sqrt(all_second) + 1e-08)).astype(jnp.bfloat16)
    directions = copy_for_each(directions, TP[0])
    directions, all_old = lax.optimization_barrier((directions, all_old))
    directions = copy_for_each(directions, TP[1])

    directions, tiles, clip = lax.optimization_barrier((directions, tiles, clip))
    projected = tiles[:, :mine].reshape(rows, RANK)
    new_first, new_second = moments_after(clip * projected, first, second)
    direction = new_first / (jnp.sqrt(new_second) + 1e-08)
    update = jnp.dot(direction, factor.astype(jnp.float32).T, precision=lax.Precision.HIGHEST)
    new_weight = old_weight - 0.05 * update
    mine = (new_weight, update, new_first, new_second)
    directions, mine = lax.optimization_barrier((directions, mine))
    directions = directions.transpose(2, 1, 0, 3, 4).reshape(HV, RANK)
    copied = lax.dot_general(
        directions, factor, (((1,), (1,)), ((), ())), preferred_element_type=jnp.float32
    )
    copied = (all_old - 0.05 * copied).astype(jnp.bfloat16)
    return (*mine, copied)


def solution(mesh):
    finer = Mesh(mesh.devices.reshape(8, 8, mesh.shape["tp"] // 2, 2), (*FS, *TP))
    in_specs = (P(FS, None), P(FS, TP), P(FS, TP), P(TP, None), P(FS, None), P(FS, None))
    out_specs = (P(FS, TP), P(FS, TP), P(FS, None), P(FS, None), P(None, TP))
    return jax.shard_map(
        on_device, mesh=finer, in_specs=in_specs, out_specs=out_specs, check_vma=False
    )
```
